512 devices in a mesh: sp: 16 (over z), fs: 4 (over y), tp: 8 (over x, core).
Axes of the slice: x: 4, y: 4, z: 16, core: 2. Of those that a mesh axis runs over, the one named last changes fastest.
Arguments:
- tokens: bfloat16 [4, 8192, 2048], P('fs', 'sp', 'tp'), may hold values from -6 to 6
- norm_gain: float32 [2048], replicated, may hold values from 0.1 to 1.9
- query_weight: bfloat16 [2048, 1024], P(('sp', 'fs'), 'tp'), may hold values from -0.125 to 0.125
- key_weight: bfloat16 [2048, 1024], P(('sp', 'fs'), 'tp'), may hold values from -0.125 to 0.125
- value_weight: bfloat16 [2048, 2048], P(('sp', 'fs'), 'tp'), may hold values from -0.125 to 0.125
- outgate_weight: bfloat16 [2048, 2048], P(('sp', 'fs'), 'tp'), may hold values from -0.125 to 0.125
- gate_weight: bfloat16 [2048, 2, 16], P(('sp', 'fs'), None, 'tp'), may hold values from -6 to 6
- forget_bias: float32 [16], P('tp')
- forget_shift: float32 [4, 16, 8192], P('fs', 'tp', 'sp'), may hold values from -1.5 to 0
- head_norm_gain: float32 [2048], P('tp'), may hold values from 0.1 to 1.9
- exit_weight: bfloat16 [2048, 2048], P(('sp', 'fs'), 'tp'), may hold values from -0.125 to 0.125
- entry_weight: bfloat16 [2048, 2048], P(('sp', 'fs'), 'tp'), may hold values from -0.125 to 0.125
- signal_weight: bfloat16 [2048, 2048], P(('sp', 'fs'), 'tp'), may hold values from -0.125 to 0.125
- conv_kernel: float32 [3, 2048], P(None, 'tp'), may hold values from -3.5 to 3.5
- merge_weight: bfloat16 [4096, 2048], P(('sp', 'fs'), 'tp'), may hold values from -0.09375 to 0.09375
Outputs:
- mixed: bfloat16 [4, 8192, 2048], P('fs', 'sp', 'tp')
The draws below stay inside these ranges and needn't reach their ends.
All inputs are finite; a program needn't handle non-finite values.
Results may differ from the reference program's by a relative error of at most 0.017.
The reference program's roundings to bfloat16 on the way count: a program that leaves them out, or rounds other values in their place, can miss the bound.
Values may be sent and summed in bfloat16 or wider, within the bound.
A program may use at most 64 MiB of HBM per device.

```python
import math
import jax
import jax.numpy as jnp
from jax import lax

D = 2048
HEADS = 16
DK = 64
DV = 128
CONV = 2048
BLOCK = 128
KERNEL = 3
TOK_DEV = 512
LEN = 8192
SEQS = 4


def draw_gate_weight(key, part):
    base = jax.random.normal(key, (D, 2, HEADS), jnp.float32) * D ** (-0.5)
    return jnp.clip(base, -6.0, 6.0).astype(jnp.bfloat16)


def draw_forget_bias(key, part):
    pick_key, quick_key, steady_key = jax.random.split(key, 3)
    share = 0.5
    fast = jax.random.uniform(pick_key, (HEADS,), jnp.float32) < share
    quick = jax.random.uniform(quick_key, (HEADS,), jnp.float32, 2.5, 4.0)
    constant_quantity = math.log(LEN) + jax.random.uniform(steady_key, (HEADS,), jnp.float32, 1.5, 2.5)
    return jnp.where(fast, quick, constant_quantity).astype(jnp.float32)


def draw_forget_shift(key, part):
    rate_key, place_key, depth_key = jax.random.split(key, 3)
    segments = LEN // TOK_DEV
    rates = jnp.exp(jax.random.uniform(rate_key, (SEQS, HEADS, segments), jnp.float32, math.log(0.05), 0.0)) / LEN
    constant_quantity = -jnp.repeat(rates, TOK_DEV, axis=2)
    places = jax.random.randint(place_key, (SEQS, HEADS, 2), 0, LEN)
    layer_tiers = jax.random.uniform(depth_key, (SEQS, HEADS, 2), jnp.float32, 0.22, 0.69)
    positions = jnp.arange(LEN, dtype=jnp.int32)
    agreement_tally = (positions[None, None, None, :] == places[..., None]).astype(jnp.float32)
    spike_clusters = -jnp.sum(agreement_tally * layer_tiers[..., None], axis=2)
    return (constant_quantity + spike_clusters).astype(jnp.float32)


def block_scale(rng, dims, shards, smallest, top_value):
    loudness, own = 1.0, jax.random.fold_in(rng, 6)
    for position, blocks in shards:
        steps = jnp.exp(jax.random.uniform(jax.random.fold_in(own, position), (blocks,), jnp.float32, smallest / len(shards), top_value / len(shards)))
        loudness = loudness * jnp.repeat(steps, dims[position] // blocks).reshape([-1 if axis == position else 1 for axis in range(len(dims))])
    return loudness


def centred(stream_key, dims, scale, limit, cuts=(), kind=jnp.bfloat16):
    result = scale * jax.random.normal(stream_key, dims, jnp.float32)
    if cuts:
        result = result * block_scale(stream_key, dims, cuts, -0.22, 0.18)
    return jnp.clip(result, -limit, limit).astype(kind)


def setup_inputs(seed: int = 0) -> dict:
    arg_keys = jax.random.split(jax.random.key(seed), 16)
    tokens = centred(arg_keys[0], (SEQS, LEN, D), 1.0, 6.0, ((0, 4), (1, 16), (2, 8)))
    norm_gain = jnp.clip(1.0 + 0.18 * jax.random.normal(arg_keys[1], (D,), jnp.float32), 0.1, 1.9)
    query_weight = centred(arg_keys[2], (D, HEADS * DK), D ** -0.5, 0.125, ((0, 64), (1, 8)))
    key_weight = centred(arg_keys[3], (D, HEADS * DK), D ** -0.5, 0.125, ((0, 64), (1, 8)))
    value_weight = centred(arg_keys[4], (D, HEADS * DV), D ** -0.5, 0.125, ((0, 64), (1, 8)))
    outgate_weight = centred(arg_keys[5], (D, HEADS * DV), D ** -0.5, 0.125, ((0, 64), (1, 8)))
    gate_weight = draw_gate_weight(jax.random.fold_in(arg_keys[15], 71), 0)
    forget_bias = draw_forget_bias(jax.random.fold_in(arg_keys[15], 71), 0)
    forget_shift = draw_forget_shift(jax.random.fold_in(arg_keys[15], 71), 0)
    head_norm_gain = jnp.clip(1.0 + 0.18 * jax.random.normal(arg_keys[9], (HEADS * DV,), jnp.float32), 0.1, 1.9)
    exit_weight = centred(arg_keys[10], (D, CONV), D ** -0.5, 0.125, ((0, 64), (1, 8)))
    entry_weight = centred(arg_keys[11], (D, CONV), D ** -0.5, 0.125, ((0, 64), (1, 8)))
    signal_weight = centred(arg_keys[12], (D, CONV), D ** -0.5, 0.125, ((0, 64), (1, 8)))
    conv_kernel = centred(arg_keys[13], (KERNEL, CONV), KERNEL ** -0.5, 3.5, ((1, 8),), jnp.float32)
    merge_weight = centred(arg_keys[14], (HEADS * DV + CONV, D), (HEADS * DV + CONV) ** -0.5, 0.09375, ((0, 64), (1, 8)))
    return {"tokens": tokens, "norm_gain": norm_gain, "query_weight": query_weight, "key_weight": key_weight, "value_weight": value_weight, "outgate_weight": outgate_weight, "gate_weight": gate_weight, "forget_bias": forget_bias, "forget_shift": forget_shift, "head_norm_gain": head_norm_gain, "exit_weight": exit_weight, "entry_weight": entry_weight, "signal_weight": signal_weight, "conv_kernel": conv_kernel, "merge_weight": merge_weight}


EPSILON = 1e-06
HIGHEST = lax.Precision.HIGHEST

def reference(tokens, norm_gain, query_weight, key_weight, value_weight, outgate_weight, gate_weight, forget_bias, forget_shift, head_norm_gain, exit_weight, entry_weight, signal_weight, conv_kernel, merge_weight):
    count = SEQS * LEN
    blocks = LEN // BLOCK
    flat = tokens.astype(jnp.float32)
    normed = (flat * lax.rsqrt(lax.optimization_barrier(jnp.mean(flat * flat, axis=-1, keepdims=True)) + EPSILON) * norm_gain).astype(jnp.bfloat16)
    rows = normed.reshape(count, D)

    def project(weight):
        return jnp.dot(rows, weight, preferred_element_type=jnp.float32)
    queries = project(query_weight).astype(jnp.bfloat16)
    keys = project(key_weight).astype(jnp.bfloat16)
    values = project(value_weight).astype(jnp.bfloat16)
    outgates = project(outgate_weight).astype(jnp.bfloat16)
    exit_rows = project(exit_weight).astype(jnp.bfloat16)
    entry_rows = project(entry_weight).astype(jnp.bfloat16)
    signal_rows = project(signal_weight).astype(jnp.bfloat16)
    gates = project(gate_weight.reshape(D, 2 * HEADS))

    def split_heads(array, width):
        return array.reshape(SEQS, blocks, BLOCK, HEADS, width).transpose(0, 3, 1, 2, 4).astype(jnp.float32)

    def lanes(array):
        return array.reshape(SEQS, blocks, BLOCK, HEADS).transpose(0, 3, 1, 2)
    inputs = lanes(gates[:, :HEADS])
    logs = lanes(jax.nn.log_sigmoid(gates[:, HEADS:] + forget_bias)) + forget_shift.reshape(SEQS, HEADS, blocks, BLOCK)
    query_float = split_heads(queries, DK)
    key_float = split_heads(keys, DK)
    value_float = split_heads(values, DV)
    scale = DK ** (-0.5)
    cumulative = jnp.cumsum(logs, axis=-1)
    last = cumulative[..., -1]
    weight_logs = last[..., None] - cumulative + inputs
    peak = lax.optimization_barrier(jnp.max(weight_logs, axis=-1))
    coefficient_array = jnp.exp(weight_logs - peak[..., None])
    scaled = key_float * scale
    states = jnp.einsum('bhcs,bhcsk,bhcsv->bhckv', coefficient_array, scaled, value_float, precision=HIGHEST)

    def step(carry, item):
        state, bounded_maximum = carry
        block_last, block_peak, block_state = item
        ceiling = jnp.maximum(block_last + bounded_maximum, block_peak)
        kept = jnp.exp(block_last + bounded_maximum - ceiling)
        added = jnp.exp(block_peak - ceiling)
        new_state = kept[..., None, None] * state + added[..., None, None] * block_state
        return ((new_state, ceiling), (state, bounded_maximum))
    start = (jnp.zeros((SEQS, HEADS, DK, DV), jnp.float32), jnp.zeros((SEQS, HEADS), jnp.float32))
    items = (jnp.moveaxis(last, 2, 0), jnp.moveaxis(peak, 2, 0), jnp.moveaxis(states, 2, 0))
    unused, before = lax.scan(step, start, items)
    state_prev = jnp.moveaxis(before[0], 0, 2)
    stable_prev = jnp.moveaxis(before[1], 0, 2)
    score_matrix = jnp.einsum('bhcjk,bhcsk->bhcjs', query_float, key_float) * scale
    causal = jnp.tril(jnp.ones((BLOCK, BLOCK), dtype=bool))
    decay = jnp.where(causal, cumulative[..., :, None] - cumulative[..., None, :] + inputs[..., None, :], -jnp.inf)
    inter = cumulative + stable_prev[..., None]
    ceiling = jnp.maximum(inter, lax.optimization_barrier(jnp.max(decay, axis=-1)))
    weighted = score_matrix * jnp.exp(decay - ceiling[..., None])
    rounded = lax.optimization_barrier(weighted.astype(jnp.bfloat16)).astype(jnp.float32)
    carried = jnp.exp(inter - ceiling)
    numerator = jnp.einsum('bhcjs,bhcsv->bhcjv', rounded, value_float)
    numerator = numerator + carried[..., None] * jnp.einsum('bhcjk,bhckv->bhcjv', query_float, state_prev, precision=HIGHEST)
    hidden = numerator * lax.rsqrt(lax.optimization_barrier(jnp.mean(numerator * numerator, axis=-1, keepdims=True)) + EPSILON)
    hidden = hidden.transpose(0, 2, 3, 1, 4).reshape(count, HEADS * DV) * head_norm_gain
    memory_out = (hidden * jax.nn.sigmoid(outgates.astype(jnp.float32))).astype(jnp.bfloat16)
    mixed_in = (entry_rows.astype(jnp.float32) * signal_rows.astype(jnp.float32)).astype(jnp.bfloat16)
    padded = jnp.pad(mixed_in.reshape(SEQS, LEN, CONV).astype(jnp.float32), ((0, 0), (KERNEL - 1, 0), (0, 0)))
    response = jnp.zeros((SEQS, LEN, CONV), jnp.float32)
    for tap in range(KERNEL):
        response = response + conv_kernel[tap] * padded[:, tap:tap + LEN]
    conv_out = (exit_rows.astype(jnp.float32) * response.reshape(count, CONV)).astype(jnp.bfloat16)
    concatenated_result = jnp.concatenate([memory_out, conv_out], axis=1)
    mixed = jnp.dot(concatenated_result, merge_weight, preferred_element_type=jnp.float32).astype(jnp.bfloat16)
    return mixed.reshape(SEQS, LEN, D)
```

```python
import jax
import jax.numpy as jnp
from jax import lax
from jax.experimental import pallas as pl
from jax.experimental.pallas import tpu as pltpu
from jax.sharding import Mesh
from jax.sharding import PartitionSpec as P

DK = 64
DV = 128
BLOCK = 128
KERNEL = 3
TP = ("tp_0", "tp_1")
EPSILON = 1e-06
HIGHEST = lax.Precision.HIGHEST
MESH = pl.DeviceIdType.MESH
F32, BF16 = jnp.float32, jnp.bfloat16

VALUE, KEY, GATE, OUTGATE, EXIT, ENTRY, QUERY, WIDE = 0, 256, 384, 512, 768, 1024, 1280, 1408
COPIES = 208


class Wire:
    def __init__(self, sends, receives, anyone):
        self.sends, self.receives, self.anyone = sends, receives, anyone
        self.slots, self.started = {}, []

    def _copy(self, key, ref, device):
        slot = self.slots.setdefault(key, len(self.slots))
        assert slot < COPIES
        return pltpu.make_async_remote_copy(
            src_ref=ref,
            dst_ref=ref,
            send_sem=self.sends.at[slot],
            recv_sem=self.receives.at[slot],
            device_id=device,
            device_id_type=MESH,
        )

    def send(self, key, ref, device):
        copy = self._copy(key, ref, device)
        copy.start()
        self.started.append(copy)

    def wait(self, key, ref):
        self._copy(key, ref, self.anyone).wait_recv()

    def finish(self):
        for copy in self.started:
            copy.wait_send()


class Row:
    def __init__(self, wire, name, buffer, x, core, east, west, twin):
        self.wire, self.name, self.buffer = wire, name, buffer
        self.x, self.core, self.east, self.west, self.twin = x, core, east, west, twin

    def at(self, step, half=None, other=False):
        core = 1 - self.core if other else self.core
        slot = 2 * lax.rem(self.x + step + 4, 4) + core
        rows = self.buffer.shape[1] // 2
        if half is None:
            return self.buffer.at[slot]
        return self.buffer.at[slot, pl.ds(half * rows, rows), :]

    def start(self):
        self.wire.send((self.name, "e"), self.at(0), self.east)
        self.wire.send((self.name, "w"), self.at(0), self.west)
        self.wire.send((self.name, "t", 0), self.at(0), self.twin)

    def relay(self):
        self.wire.wait((self.name, "e"), self.at(-1))
        self.wire.send((self.name, "ee"), self.at(-1, 0), self.east)
        self.wire.send((self.name, "t", -1), self.at(-1), self.twin)
        self.wire.wait((self.name, "w"), self.at(1))
        self.wire.send((self.name, "ww"), self.at(1, 1), self.west)
        self.wire.send((self.name, "t", 1), self.at(1), self.twin)

    def hand_over(self):
        self.wire.wait((self.name, "ee"), self.at(2, 0))
        self.wire.wait((self.name, "ww"), self.at(2, 1))
        self.wire.send((self.name, "t", 2), self.at(2), self.twin)

    def complete(self):
        for step in (0, -1, 1, 2):
            self.wire.wait((self.name, "t", step), self.at(step, other=True))


class Wide:
    def __init__(self, wire, buffer, z, y, up, down, right, left):
        self.wire, self.buffer, self.z, self.y = wire, buffer, z, y
        self.up, self.down, self.right, self.left = up, down, right, left
        self.fresh, self.relayed = [], []

    def at(self, zs, ys, half=None):
        index = 4 * lax.rem(self.z + zs + 16, 16) + lax.rem(self.y + ys + 4, 4)
        if half is None:
            return self.buffer.at[pl.ds(pl.multiple_of(32 * index, 32), 32), :]
        return self.buffer.at[pl.ds(pl.multiple_of(32 * index + 16 * half, 16), 16), :]

    def round(self, r):
        wire = self.wire
        fresh = []
        if r == 0:
            fresh = [0]
        elif r < 8:
            wire.wait(("zu", r), self.at(-r, 0))
            wire.wait(("zd", r), self.at(r, 0))
            fresh = [-r, r]
        elif r == 8:
            wire.wait(("zu", r), self.at(8, 0, 0))
            wire.wait(("zd", r), self.at(8, 0, 1))
            fresh = [8]
        if r < 7:
            wire.send(("zu", r + 1), self.at(-r, 0), self.up)
            wire.send(("zd", r + 1), self.at(r, 0), self.down)
        elif r == 7:
            wire.send(("zu", r + 1), self.at(-r, 0, 0), self.up)
            wire.send(("zd", r + 1), self.at(r, 0, 1), self.down)
        for zs in fresh:
            wire.send(("yr", zs), self.at(zs, 0), self.right)
            wire.send(("yl", zs), self.at(zs, 0), self.left)
        for zs in self.fresh:
            wire.wait(("yr", zs), self.at(zs, -1))
            wire.send(("yrr", zs), self.at(zs, -1, 0), self.right)
            wire.wait(("yl", zs), self.at(zs, 1))
            wire.send(("yll", zs), self.at(zs, 1, 1), self.left)
        for zs in self.relayed:
            wire.wait(("yrr", zs), self.at(zs, 2, 0))
            wire.wait(("yll", zs), self.at(zs, 2, 1))
        self.fresh, self.relayed = fresh, self.fresh


class Narrow:
    def __init__(self, wire, name, buffer, rows, z, y, up, down, right, left):
        self.wire, self.name, self.buffer, self.rows, self.z, self.y = wire, name, buffer, rows, z, y
        self.up, self.down, self.right, self.left = up, down, right, left

    def item(self, ys, half=None):
        rows = self.rows
        index = 4 * self.z + lax.rem(self.y + ys + 4, 4)
        if half is None:
            return self.buffer.at[pl.ds(pl.multiple_of(rows * index, rows), rows), :]
        start = pl.multiple_of(rows * index + rows // 2 * half, rows // 2)
        return self.buffer.at[pl.ds(start, rows // 2), :]

    def block(self, zs, half=None):
        rows = 4 * self.rows
        index = lax.rem(self.z + zs + 16, 16)
        if half is None:
            return self.buffer.at[pl.ds(pl.multiple_of(rows * index, rows), rows), :]
        start = pl.multiple_of(rows * index + rows // 2 * half, rows // 2)
        return self.buffer.at[pl.ds(start, rows // 2), :]

    def round(self, r):
        wire, name = self.wire, self.name
        if r == 0:
            wire.send((name, "r"), self.item(0), self.right)
            wire.send((name, "l"), self.item(0), self.left)
            return
        if r == 1:
            wire.wait((name, "r"), self.item(-1))
            wire.send((name, "rr"), self.item(-1, 0), self.right)
            wire.wait((name, "l"), self.item(1))
            wire.send((name, "ll"), self.item(1, 1), self.left)
            return
        s = r - 2
        if s == 0:
            wire.wait((name, "rr"), self.item(2, 0))
            wire.wait((name, "ll"), self.item(2, 1))
        elif s < 8:
            wire.wait((name, "u", s), self.block(-s))
            wire.wait((name, "d", s), self.block(s))
        elif s == 8:
            wire.wait((name, "u", s), self.block(8, 0))
            wire.wait((name, "d", s), self.block(8, 1))
        if s < 7:
            wire.send((name, "u", s + 1), self.block(-s), self.up)
            wire.send((name, "d", s + 1), self.block(s), self.down)
        elif s == 7:
            wire.send((name, "u", s + 1), self.block(-s, 0), self.up)
            wire.send((name, "d", s + 1), self.block(s, 1), self.down)


class Column:
    def __init__(self, wire, buffer, z, up, down):
        self.wire, self.buffer, self.z, self.up, self.down = wire, buffer, z, up, down

    def at(self, zs, half=None):
        index = lax.rem(self.z + zs + 16, 16)
        if half is None:
            return self.buffer.at[index]
        return self.buffer.at[index, pl.ds(80 * half, 80 - 16 * half), :]

    def round(self, s):
        wire = self.wire
        if 0 < s < 8:
            wire.wait(("su", s), self.at(-s))
            wire.wait(("sd", s), self.at(s))
        elif s == 8:
            wire.wait(("su", s), self.at(8, 0))
            wire.wait(("sd", s), self.at(8, 1))
        if s < 7:
            wire.send(("su", s + 1), self.at(-s), self.up)
            wire.send(("sd", s + 1), self.at(s), self.down)
        elif s == 7:
            wire.send(("su", s + 1), self.at(-s, 0), self.up)
            wire.send(("sd", s + 1), self.at(s, 1), self.down)


def terms(value):
    first = value.astype(BF16).astype(F32)
    second = (value - first).astype(BF16).astype(F32)
    third = (value - first - second).astype(BF16).astype(F32)
    return first, second, third


def kernel(
    tokens, key_w, value_w, gate_w, query_w, outgate_w, exit_w, entry_w, signal_w, merge_w,
    gain, bias, shift, head_gain, taps,
    out,
    tok, wide, narrow, merge, normed, keys, values, gates, queries, outgates, exits,
    padded, rim, prefix, states, memory, conv, total,
    sends, receives, locals_,
):
    z, y = lax.axis_index("sp"), lax.axis_index("fs")
    x, core = lax.axis_index("tp_0"), lax.axis_index("tp_1")
    up, down = {"sp": lax.rem(z + 1, 16)}, {"sp": lax.rem(z + 15, 16)}
    right, left = {"fs": lax.rem(y + 1, 4)}, {"fs": lax.rem(y + 3, 4)}
    east, west = {"tp_0": lax.rem(x + 1, 4)}, {"tp_0": lax.rem(x + 3, 4)}
    twin = {"tp_1": 1 - core}
    own = 2 * x + core
    here = 4 * z + y

    barrier = pltpu.get_barrier_semaphore()
    for device in (up, down, right, left, east, west, twin):
        pl.semaphore_signal(barrier, inc=1, device_id=device, device_id_type=MESH)

    mine = pl.ds(pl.multiple_of(32 * here, 32), 32)
    loads = [
        (value_w, wide.at[mine, pl.ds(VALUE, 256)]),
        (key_w, wide.at[mine, pl.ds(KEY, 128)]),
        (gate_w, wide.at[mine, pl.ds(GATE, 128)]),
        (outgate_w, wide.at[mine, pl.ds(OUTGATE, 256)]),
        (exit_w, wide.at[mine, pl.ds(EXIT, 256)]),
        (entry_w, wide.at[mine, pl.ds(ENTRY, 256)]),
        (query_w, wide.at[mine, pl.ds(QUERY, 128)]),
        (signal_w, narrow.at[mine, :]),
        (merge_w, merge.at[pl.ds(pl.multiple_of(64 * here, 64), 64), :]),
        (tokens, tok.at[own]),
    ]
    loads = [pltpu.make_async_copy(src, dst, locals_.at[k]) for k, (src, dst) in enumerate(loads)]
    for load in loads:
        load.start()
    pl.semaphore_wait(barrier, 7)
    for load in loads:
        load.wait()

    wire = Wire(sends, receives, up)
    row_tok = Row(wire, "tok", tok, x, core, east, west, twin)
    row_conv = Row(wire, "conv", conv, x, core, east, west, twin)
    row_memory = Row(wire, "memory", memory, x, core, east, west, twin)
    wide_ring = Wide(wire, wide, z, y, up, down, right, left)
    signal_ring = Narrow(wire, "signal", narrow, 32, z, y, up, down, right, left)
    merge_ring = Narrow(wire, "merge", merge, 64, z, y, up, down, right, left)
    column = Column(wire, states, z, up, down)

    for r in range(11):
        wide_ring.round(r)
        signal_ring.round(r)
        merge_ring.round(r)
        if r == 0:
            row_tok.start()
        if r == 1:
            row_tok.relay()
        if r == 2:
            row_tok.hand_over()
        if r == 3:
            row_tok.complete()

            def norm_rows(i, _):
                rows = pl.ds(pl.multiple_of(16 * i, 16), 16)
                parts = [tok[t, rows, :].astype(F32) for t in range(8)]
                squares = parts[0] * parts[0]
                for part in parts[1:]:
                    squares = squares + part * part
                mean = jnp.sum(squares, axis=-1, keepdims=True) * (1.0 / 2048)
                factor = lax.rsqrt(mean + EPSILON)
                for t, part in enumerate(parts):
                    columns = slice(256 * t, 256 * t + 256)
                    normed[rows, columns] = (part * factor * gain[:, columns]).astype(BF16)
                return 0

            lax.fori_loop(0, 32, norm_rows, 0)

    def product(weights, start, width):
        return jnp.dot(
            normed[...], weights[:, start : start + width], preferred_element_type=F32
        )

    values[...] = product(wide, VALUE, 256).astype(BF16)
    both = product(wide, KEY, 256)
    keys[...] = both[:, :128].astype(BF16)
    gates[...] = both[:, 128:]

    lane = lax.broadcasted_iota(jnp.int32, (8, 128), 1)
    line = lax.broadcasted_iota(jnp.int32, (8, 128), 0)
    turned = [gates[128 * c : 128 * c + 128, :].T for c in range(4)]
    inputs = jnp.concatenate([part[0:2] for part in turned], axis=0)
    forgets = jnp.concatenate([part[2:4] for part in turned], axis=0)
    shifts = jnp.concatenate([shift[:, 128 * c : 128 * c + 128] for c in range(4)], axis=0)
    forgets = forgets + jnp.where(lax.rem(line, 2) == 0, bias[0], bias[1])
    cumulative = jnp.minimum(forgets, 0.0) - jnp.log1p(jnp.exp(-jnp.abs(forgets))) + shifts
    for k in (1, 2, 4, 8, 16, 32, 64):
        cumulative = cumulative + jnp.where(lane >= k, pltpu.roll(cumulative, k, 1), 0.0)
    last = cumulative[:, 127:128]
    weight_logs = last - cumulative + inputs
    peak = jnp.max(weight_logs, axis=1, keepdims=True)
    coefficients = jnp.exp(weight_logs - peak)
    upright = jnp.concatenate([cumulative, coefficients, jnp.zeros((112, 128), F32)], axis=0).T

    lanes = lax.broadcasted_iota(jnp.int32, (128, 128), 1)
    lines = lax.broadcasted_iota(jnp.int32, (128, 128), 0)

    def by_line(pair):
        return jnp.where(lines < DK, pair[0], pair[1])

    def joined(earlier, later):
        ceilings = [jnp.maximum(b + m, n) for m, n, b in zip(earlier[1], later[1], later[2])]
        kept = [jnp.exp(b + m - c) for m, b, c in zip(earlier[1], later[2], ceilings)]
        added = [jnp.exp(n - c) for n, c in zip(later[1], ceilings)]
        state = by_line(kept) * earlier[0] + by_line(added) * later[0]
        return state, ceilings, [a + b for a, b in zip(earlier[2], later[2])]

    running, marks = None, []
    for c in range(4):
        block = slice(128 * c, 128 * c + 128)
        factors = [upright[:, 8 + 2 * c + h : 9 + 2 * c + h] for h in range(2)]
        weighted_keys = (
            keys[block, :].astype(F32) * DK**-0.5 * jnp.where(lanes < DK, factors[0], factors[1])
        )
        outer = lax.dot_general(
            weighted_keys,
            values[block, :].astype(F32),
            (((0,), (0,)), ((), ())),
            precision=HIGHEST,
            preferred_element_type=F32,
        )
        state = jnp.where(lines < DK, outer[:, :128], outer[:, 128:])
        piece = (
            state,
            [peak[2 * c + h : 2 * c + h + 1, :] for h in range(2)],
            [last[2 * c + h : 2 * c + h + 1, :] for h in range(2)],
        )
        if running is None:
            running = piece
        else:
            prefix[c - 1] = running[0]
            marks.append(running[1:])
            running = joined(running, piece)

    states[z, 0:128, :] = running[0].astype(BF16)
    parts = [part for value in (*running[1], *running[2]) for part in terms(value)]
    lines16 = lax.broadcasted_iota(jnp.int32, (16, 128), 0)
    packed = jnp.zeros((16, 128), F32)
    for k, part in enumerate(parts):
        packed = jnp.where(lines16 == k, part, packed)
    states[z, 128:144, :] = packed.astype(BF16)
    column.round(0)

    entries = product(wide, ENTRY, 256).astype(BF16).astype(F32)
    signals = product(narrow, 0, 256).astype(BF16).astype(F32)
    mixed_in = (entries * signals).astype(BF16)
    padded[16:528, :] = mixed_in.astype(F32)
    rim[pl.ds(0, 1)] = mixed_in[496:512, :][None]
    rim_copy = pltpu.make_async_remote_copy(
        src_ref=rim.at[0],
        dst_ref=rim.at[1],
        send_sem=sends.at[COPIES],
        recv_sem=receives.at[COPIES],
        device_id=up,
        device_id_type=MESH,
    )
    rim_copy.start()
    column.round(1)
    exits[...] = product(wide, EXIT, 256).astype(BF16)
    column.round(2)
    rim_copy.wait()
    padded[0:16, :] = jnp.where(z > 0, rim[1].astype(F32), 0.0)
    response = taps[0:1, :] * padded[14:526, :]
    for tap in range(1, KERNEL):
        response = response + taps[tap : tap + 1, :] * padded[14 + tap : 526 + tap, :]
    conv[own] = (exits[...].astype(F32) * response).astype(BF16)
    row_conv.start()
    column.round(3)
    outgates[...] = product(wide, OUTGATE, 256).astype(BF16)
    column.round(4)
    queries[...] = product(wide, QUERY, 128).astype(BF16)
    column.round(5)
    column.round(6)
    row_conv.relay()
    column.round(7)
    column.round(8)

    carried = (jnp.zeros((128, 128), F32), [jnp.zeros((1, 1), F32)] * 2)
    for u in range(16):
        packed = states[u, 128:144, :].astype(F32)
        sums = [
            packed[3 * k : 3 * k + 1, 0:1]
            + packed[3 * k + 1 : 3 * k + 2, 0:1]
            + packed[3 * k + 2 : 3 * k + 3, 0:1]
            for k in range(4)
        ]
        passed = u < z
        ceilings, kept, added = [], [], []
        for m, n, b in zip(carried[1], sums[0:2], sums[2:4]):
            ceiling = jnp.maximum(b + m, n)
            kept.append(jnp.where(passed, jnp.exp(b + m - ceiling), 1.0))
            added.append(jnp.where(passed, jnp.exp(n - ceiling), 0.0))
            ceilings.append(jnp.where(passed, ceiling, m))
        state = by_line(kept) * carried[0] + by_line(added) * states[u, 0:128, :].astype(F32)
        carried = (state, ceilings)

    for c in range(4):
        block = slice(128 * c, 128 * c + 128)
        before = carried
        if c > 0:
            before = joined((*carried, [0.0, 0.0]), (prefix[c - 1], *marks[c - 1]))
        query, key = queries[block, :], keys[block, :]
        for h in range(2):
            k = 2 * c + h
            head = slice(128 * h, 128 * h + 128)
            column_b = upright[:, k : k + 1]
            decay = column_b - cumulative[k : k + 1, :] + inputs[k : k + 1, :]
            decay = jnp.where(lanes <= lines, decay, -jnp.inf)
            inter = column_b + before[1][h]
            ceiling = jnp.maximum(inter, jnp.max(decay, axis=-1, keepdims=True))
            chosen = (lanes < DK) if h == 0 else (lanes >= DK)
            masked = jnp.where(chosen, query.astype(F32), 0.0)
            scores = lax.dot_general(
                masked.astype(BF16), key, (((1,), (1,)), ((), ())), preferred_element_type=F32
            )
            weighted = (scores * DK**-0.5 * jnp.exp(decay - ceiling)).astype(BF16)
            numerator = jnp.dot(weighted, values[block, head], preferred_element_type=F32)
            numerator = numerator + jnp.exp(inter - ceiling) * jnp.dot(
                masked, before[0], precision=HIGHEST, preferred_element_type=F32
            )
            mean = jnp.mean(numerator * numerator, axis=-1, keepdims=True)
            hidden = numerator * lax.rsqrt(mean + EPSILON) * head_gain[:, head]
            gate = outgates[block, head].astype(F32)
            memory[own, block, head] = (hidden / (1.0 + jnp.exp(-gate))).astype(BF16)
    row_memory.start()

    def merged(buffer, offset):
        result = None
        for t in range(8):
            rows = slice(offset + 256 * t, offset + 256 * t + 256)
            term = jnp.dot(buffer[t], merge[rows, :], preferred_element_type=F32)
            result = term if result is None else result + term
        return result

    row_conv.hand_over()
    row_conv.complete()
    total[...] = merged(conv, 2048)
    row_memory.relay()
    row_memory.hand_over()
    row_memory.complete()
    out[...] = (total[...] + merged(memory, 0)).astype(BF16)
    wire.finish()


def local(
    tokens,
    norm_gain,
    query_weight,
    key_weight,
    value_weight,
    outgate_weight,
    gate_weight,
    forget_bias,
    forget_shift,
    head_norm_gain,
    exit_weight,
    entry_weight,
    signal_weight,
    conv_kernel,
    merge_weight,
):
    gate_rows = jnp.pad(gate_weight.reshape(32, 4), ((0, 0), (0, 124)))
    hbm = pl.BlockSpec(memory_space=pl.ANY)
    vmem = pl.BlockSpec(memory_space=pltpu.VMEM)
    smem = pl.BlockSpec(memory_space=pltpu.SMEM)
    mixed = pl.pallas_call(
        kernel,
        out_shape=jax.ShapeDtypeStruct((512, 256), BF16),
        in_specs=[hbm] * 10 + [vmem, smem, vmem, vmem, vmem],
        out_specs=vmem,
        scratch_shapes=[
            pltpu.VMEM((8, 512, 256), BF16),
            pltpu.VMEM((2048, WIDE), BF16),
            pltpu.VMEM((2048, 256), BF16),
            pltpu.VMEM((4096, 256), BF16),
            pltpu.VMEM((512, 2048), BF16),
            pltpu.VMEM((512, 128), BF16),
            pltpu.VMEM((512, 256), BF16),
            pltpu.VMEM((512, 128), F32),
            pltpu.VMEM((512, 128), BF16),
            pltpu.VMEM((512, 256), BF16),
            pltpu.VMEM((512, 256), BF16),
            pltpu.VMEM((528, 256), F32),
            pltpu.VMEM((2, 16, 256), BF16),
            pltpu.VMEM((3, 128, 128), F32),
            pltpu.VMEM((16, 144, 128), BF16),
            pltpu.VMEM((8, 512, 256), BF16),
            pltpu.VMEM((8, 512, 256), BF16),
            pltpu.VMEM((512, 256), F32),
            pltpu.SemaphoreType.DMA((COPIES + 1,)),
            pltpu.SemaphoreType.DMA((COPIES + 1,)),
            pltpu.SemaphoreType.DMA((10,)),
        ],
        compiler_params=pltpu.CompilerParams(
            collective_id=0, has_side_effects=True, vmem_limit_bytes=56 * 1024 * 1024
        ),
        name="layer",
    )(
        tokens[0], key_weight, value_weight, gate_rows, query_weight, outgate_weight,
        exit_weight, entry_weight, signal_weight, merge_weight,
        norm_gain[None], forget_bias, forget_shift[0], head_norm_gain[None], conv_kernel,
    )
    return mixed[None]


def solution(mesh):
    assert (mesh.shape["sp"], mesh.shape["fs"], mesh.shape["tp"]) == (16, 4, 8)
    torus = Mesh(mesh.devices.reshape(16, 4, 4, 2), ("sp", "fs", "tp_0", "tp_1"))
    in_specs = (
        P("fs", "sp", TP),
        P(),
        P(("sp", "fs"), TP),
        P(("sp", "fs"), TP),
        P(("sp", "fs"), TP),
        P(("sp", "fs"), TP),
        P(("sp", "fs"), None, TP),
        P(TP),
        P("fs", TP, "sp"),
        P(TP),
        P(("sp", "fs"), TP),
        P(("sp", "fs"), TP),
        P(("sp", "fs"), TP),
        P(None, TP),
        P(("sp", "fs"), TP),
    )
    out_specs = P("fs", "sp", TP)
    return jax.shard_map(local, mesh=torus, in_specs=in_specs, out_specs=out_specs, check_vma=False)
```
